32 devices in a mesh: ep: 8 (over z, x), tp: 4 (over y, core).
Axes of the slice: x: 2, y: 2, z: 4, core: 2. Of those that a mesh axis runs over, the one named last changes fastest.
Arguments:
- tokens: bfloat16 [8192, 2048], P(('ep', 'tp')), may hold values from -6 to 6
- norm_gain: bfloat16 [2048], replicated, may hold values from 0.099609375 to 1.8984375
- expert_ids: int32 [8192, 2], P(('ep', 'tp')), may hold values from 0 to 7, all different within a row; in each aligned block of 256 rows (0 to 255, 256 to 511, ...) at most 128 rows name the same one
- group_weight: float32 [8192], P(('ep', 'tp')), may hold values from 0.25 to 1
- expert_logit: float32 [8192, 2], P(('ep', 'tp')), may hold values from -4 to 4
- w_gate: bfloat16 [8, 2048, 1024], P('ep', None, 'tp'), may hold values from -0.125 to 0.125
- w_up: bfloat16 [8, 2048, 1024], P('ep', None, 'tp'), may hold values from -0.125 to 0.125
- w_down: bfloat16 [8, 1024, 2048], P('ep', 'tp')
- final_gain: bfloat16 [2048], P('tp'), may hold values from 0.099609375 to 1.8984375
Outputs:
- normed_out: bfloat16 [8192, 2048], P('ep', 'tp')
The draws below stay inside these ranges and needn't reach their ends.
Inputs may be any that keep to these rules, and one draw needn't show every extreme that they name: `expert_ids`: the 2 experts of a token differ. Among the rows of one device (aligned blocks of 256 tokens) no expert is named more than 128 times, a bound that some block reaches.
All inputs are finite; a program needn't handle non-finite values.
Results may differ from the reference program's by a relative error of at most 0.0058.
Values may be sent and summed in bfloat16 or wider, within the bound.
A program may use at most 128 MiB of HBM per device.

```python
import math
import jax
import jax.numpy as jnp
import numpy as np
from jax import lax

D = 2048
FF = 1024
TOP = 2
TOK_DEV = 256
EXPERTS = 8
CAP = 128
TOKENS = 8192


def draw_w_down(key, part):
    first, second = jax.random.split(key)
    base = jax.random.normal(first, (EXPERTS, FF, D), jnp.float32)
    levels = jnp.array([0.4, 0.9, 1.5, 2.4], jnp.float32)
    shuffled = levels[jax.random.permutation(second, 4)]
    quarter = jnp.arange(D, dtype=jnp.int32) * 4 // D
    column_scale = shuffled[quarter]
    return (base * FF ** (-0.5) * column_scale[None, None, :]).astype(jnp.bfloat16)


def block_levels(stream_key, extent, shards, smallest, largest):
    loudness, own = 1.0, jax.random.fold_in(stream_key, 6)
    for position, blocks in shards:
        heights = jnp.exp(jax.random.uniform(jax.random.fold_in(own, position), (blocks,), jnp.float32, smallest / len(shards), largest / len(shards)))
        loudness = loudness * jnp.repeat(heights, extent[position] // blocks).reshape([-1 if axis == position else 1 for axis in range(len(extent))])
    return loudness


def shared_out(key, own, number, rows, number_of, top, limit, slope):
    ranking = jax.random.permutation(key, number_of)
    packed, common = shares(number_of, rows * top, limit, slope, True), shares(number_of, rows * top, limit, slope, False)
    places = jnp.arange(number_of)

    def named(tallies, rotation):
        used = int((tallies > 0).sum())
        fixed = max(1, used // 4)
        passed = fixed + (places - fixed + rotation * (used - fixed)) % max(1, number_of - fixed)
        return jnp.zeros((number_of,), jnp.int32).at[ranking[jnp.where(places < fixed, places, passed)]].set(jnp.asarray(tallies, jnp.int32))

    tallies = jnp.where(number % 4 == 0, named(packed, number // 4), named(common, number - number // 4 - 1))
    mixed = jax.random.permutation(jax.random.fold_in(own, 3), number_of)
    giver, sink = mixed[0:number_of // 2 * 2:2], mixed[1:number_of // 2 * 2:2]
    slack = jnp.minimum(tallies[giver] - 1, limit - tallies[sink]) // 2
    slack = jnp.where((giver == ranking[0]) | (sink == ranking[0]) | (tallies[sink] == 0), 0, jnp.maximum(slack, 0))
    passed = jax.random.randint(jax.random.fold_in(own, 4), (number_of // 2,), 0, 1 << 20) % (slack + 1)
    tallies = tallies.at[giver].add(-passed).at[sink].add(passed)
    labels = jnp.searchsorted(jnp.cumsum(tallies), jnp.arange(rows * top), side="right").astype(jnp.int32)
    grid = labels.reshape(top, rows).T
    grid = grid[jax.random.permutation(jax.random.fold_in(own, 1), rows)]
    rotation = jax.random.randint(jax.random.fold_in(own, 2), (rows, 1), 0, top)
    return jnp.take_along_axis(grid, (jnp.arange(top)[None, :] + rotation) % top, axis=1)


def shares(count, total, reach, slope, full):
    loads = [(1 << 20) // math.isqrt(standing ** slope) + 1 for standing in range(1, count + 1)]
    largest = reach if full else min(reach, max(-(-total // count), total * loads[0] // sum(loads)))
    least = 1 if total - largest >= count - 1 else 0
    holding, spare = [largest] + [least] * (count - 1), total - largest - least * (count - 1)
    while spare > 0:
        candidates = [i for i in range(1, count) if holding[i] < largest] or [i for i in range(1, count) if holding[i] < reach]
        mass, remaining = sum([loads[i] for i in candidates]), spare
        for i in candidates:
            more = min(reach - holding[i], max(1, remaining * loads[i] // mass), spare)
            holding[i] = holding[i] + more
            spare = spare - more
    return np.array(holding)


def noise(key, dims, deviation, most, cuts=(), held_as=jnp.bfloat16):
    values = jax.random.normal(key, dims, jnp.float32) * deviation
    if len(cuts) > 0:
        values = block_levels(key, dims, cuts, -0.22, 0.18) * values
    return jnp.clip(values, min=-most, max=most).astype(held_as)


def setup_inputs(seed: int = 0) -> dict:
    key_list = jax.random.split(jax.random.key(seed), 10)
    tokens = noise(key_list[0], (TOKENS, D), 1.0, 6.0, ((0, 32),))
    norm_gain = jnp.clip(1.0 + 0.18 * jax.random.normal(key_list[1], (D,), jnp.float32), 0.099609375, 1.8984375).astype(jnp.bfloat16)
    expert_ids_keys = jax.random.split(jax.random.fold_in(key_list[2], 1), TOKENS // TOK_DEV)
    expert_ids_turns = jax.random.permutation(jax.random.fold_in(key_list[2], 3), TOKENS // TOK_DEV)
    expert_ids = jax.vmap(lambda own, number: shared_out(jax.random.fold_in(key_list[2], 2), own, number, TOK_DEV, EXPERTS, TOP, CAP, 2))(expert_ids_keys, expert_ids_turns).reshape((TOKENS, TOP))
    group_weight = jnp.clip(0.25 + 0.75 * jax.random.uniform(key_list[3], (TOKENS,), jnp.float32) ** block_levels(key_list[3], (TOKENS,), ((0, 32),), -0.2, 0.2), 0.25, 1.0)
    expert_logit = noise(key_list[4], (TOKENS, TOP), 1.5, 4.0, ((0, 32),), jnp.float32)
    w_gate = noise(key_list[5], (EXPERTS, D, FF), D ** -0.5, 0.125, ((0, 8), (2, 4)))
    w_up = noise(key_list[6], (EXPERTS, D, FF), D ** -0.5, 0.125, ((0, 8), (2, 4)))
    w_down = draw_w_down(jax.random.fold_in(key_list[9], 71), 0)
    final_gain = jnp.clip(1.0 + 0.18 * jax.random.normal(key_list[8], (D,), jnp.float32), 0.099609375, 1.8984375).astype(jnp.bfloat16)
    return dict(tokens=tokens, norm_gain=norm_gain, expert_ids=expert_ids, group_weight=group_weight, expert_logit=expert_logit, w_gate=w_gate, w_up=w_up, w_down=w_down, final_gain=final_gain)


EPS = 1e-06

def normalize(values, gain):
    return values * lax.rsqrt(lax.optimization_barrier(jnp.mean(values * values, axis=-1, keepdims=True)) + EPS) * gain.astype(jnp.float32)

def reference(tokens, norm_gain, expert_ids, group_weight, expert_logit, w_gate, w_up, w_down, final_gain):
    block_len = 256
    tokens_f = tokens.astype(jnp.float32)
    normed_in = normalize(tokens_f, norm_gain).astype(jnp.bfloat16)
    total_tok, per_token = expert_ids.shape
    experts = w_gate.shape[0]
    assigned = total_tok * per_token
    flat_ids = expert_ids.reshape(assigned).astype(jnp.int32)
    sort_order = jnp.argsort(flat_ids, stable=True).astype(jnp.int32)
    sorted_ids = flat_ids[sort_order]
    counts = jnp.bincount(flat_ids, length=experts).astype(jnp.int32)
    starts = (jnp.cumsum(counts) - counts).astype(jnp.int32)
    padded = (counts + block_len - 1) // block_len * block_len
    ends = jnp.cumsum(padded).astype(jnp.int32)
    pad_starts = (ends - padded).astype(jnp.int32)
    target = (pad_starts[sorted_ids] + jnp.arange(assigned, dtype=jnp.int32) - starts[sorted_ids]).astype(jnp.int32)
    blocks = assigned // block_len + experts + 1
    row_token = jnp.zeros((blocks * block_len,), jnp.int32).at[target].set((sort_order // per_token).astype(jnp.int32))
    block_expert = jnp.minimum(jnp.searchsorted(ends, jnp.arange(blocks, dtype=jnp.int32) * block_len, side='right'), experts - 1).astype(jnp.int32)
    inputs = normed_in[row_token].reshape(blocks, block_len, normed_in.shape[1])

    def expert_block(pair):
        rows, which = pair
        gate = jnp.dot(rows, w_gate[which], preferred_element_type=jnp.float32)
        upper = jnp.dot(rows, w_up[which], preferred_element_type=jnp.float32)
        hidden = (jax.nn.silu(gate) * upper).astype(jnp.bfloat16)
        return jnp.dot(hidden, w_down[which], preferred_element_type=jnp.float32).astype(jnp.bfloat16)
    outputs = lax.map(expert_block, (inputs, block_expert)).reshape(blocks * block_len, normed_in.shape[1])
    where_row = jnp.zeros((assigned,), jnp.int32).at[sort_order].set(target).reshape(total_tok, per_token)
    expert_share = jnp.exp(expert_logit)
    expert_share = expert_share / lax.optimization_barrier(jnp.sum(expert_share, axis=-1, keepdims=True))
    route_weight = group_weight[:, None] * expert_share
    mixture = tokens_f
    for member in range(per_token):
        mixture = mixture + route_weight[:, member:member + 1] * outputs[where_row[:, member]].astype(jnp.float32)
    residual = mixture.astype(jnp.bfloat16).astype(jnp.float32)
    return normalize(residual, final_gain).astype(jnp.bfloat16)
```

```python
import functools

import jax
import jax.numpy as jnp
from jax import lax
from jax.experimental import pallas as pl
from jax.experimental.pallas import tpu as pltpu
from jax.sharding import PartitionSpec as P

EPS = 1e-06
PAIR = 2
MESH = pl.DeviceIdType.MESH
VMEM = pl.BlockSpec(memory_space=pltpu.VMEM)


def line_gather(line, parts, x_ref, m_ref, o_ref, mo_ref, right_sem, left_sem, recv_sem,
                mright_sem, mleft_sem, mrecv_sem):
    ep = lax.axis_index("ep")
    z = ep // PAIR
    rows = x_ref.shape[0] // parts
    barrier = pltpu.get_barrier_semaphore()

    @pl.when(z > 0)
    def _():
        pl.semaphore_signal(barrier, inc=1, device_id={"ep": ep - PAIR}, device_id_type=MESH)

    @pl.when(z < line - 1)
    def _():
        pl.semaphore_signal(barrier, inc=1, device_id={"ep": ep + PAIR}, device_id_type=MESH)

    pl.semaphore_wait(barrier, jnp.where(z > 0, 1, 0) + jnp.where(z < line - 1, 1, 0))

    def copy(step, part, block, target, sems):
        piece = pl.ds(part * rows, rows)
        source = x_ref.at[piece] if step == 0 else o_ref.at[block, piece]
        return pltpu.make_async_remote_copy(
            src_ref=source, dst_ref=o_ref.at[block, piece], send_sem=sems.at[block, part],
            recv_sem=recv_sem.at[block, part], device_id={"ep": target}, device_id_type=MESH)

    def copy_meta(step, block, target, sems):
        source = m_ref if step == 0 else mo_ref.at[block]
        return pltpu.make_async_remote_copy(
            src_ref=source, dst_ref=mo_ref.at[block], send_sem=sems.at[block],
            recv_sem=mrecv_sem.at[block], device_id={"ep": target}, device_id_type=MESH)

    for step in range(line - 1):
        for part in range(parts):
            for way, sems, msems in ((1, right_sem, mright_sem), (-1, left_sem, mleft_sem)):
                block = z - way * step
                target = ep + way * PAIR
                here = (block >= 0) & (block < line)
                there = (z + way >= 0) & (z + way < line)
                if step > 0:
                    @pl.when(here)
                    def _():
                        copy(step, part, block, target, sems).wait_recv()
                        if part == 0:
                            copy_meta(step, block, target, msems).wait_recv()

                @pl.when(here & there)
                def _():
                    if part == 0:
                        copy_meta(step, block, target, msems).start()
                    copy(step, part, block, target, sems).start()
        if step == 0:
            o_ref[z] = x_ref[...]
            mo_ref[z] = m_ref[...]
    for way, sems, msems in ((1, right_sem, mright_sem), (-1, left_sem, mleft_sem)):
        last = z - way * (line - 1)

        @pl.when((last >= 0) & (last < line))
        def _():
            copy_meta(1, last, ep, msems).wait_recv()
            for part in range(parts):
                copy(1, part, last, ep, sems).wait_recv()

        for step in range(line - 1):
            block = z - way * step

            @pl.when((block >= 0) & (block < line) & (z + way >= 0) & (z + way < line))
            def _():
                copy_meta(step, block, ep, msems).wait_send()
                for part in range(parts):
                    copy(step, part, block, ep, sems).wait_send()


def experts_kernel(line, cap, x_ref, m_ref, gate_ref, up_ref, down_ref, o_ref, rows_ref, acc_ref,
                   pick_ref, weight_ref, part_ref):
    e, j = pl.program_id(0), pl.program_id(1)
    last_e, last_j = pl.num_programs(0) - 1, pl.num_programs(1) - 1
    tok = x_ref.shape[1]

    @pl.when(j == 0)
    def _():
        expert = (lax.axis_index("ep") // PAIR * PAIR + e).astype(jnp.float32)
        earlier = (lax.broadcasted_iota(jnp.int32, (tok, tok), 0)
                   < lax.broadcasted_iota(jnp.int32, (tok, tok), 1)).astype(jnp.bfloat16)
        slot = lax.broadcasted_iota(jnp.int32, (cap, tok), 0).astype(jnp.float32)
        for b in range(line):
            meta = m_ref[b]
            first, second = meta[0:1] == expert, meta[1:2] == expert
            named = jnp.where(first | second, 1.0, 0.0)
            share = jnp.where(first, meta[2:3], 0.0) + jnp.where(second, meta[3:4], 0.0)
            rank = jnp.dot(jnp.broadcast_to(named, (8, tok)).astype(jnp.bfloat16), earlier,
                           preferred_element_type=jnp.float32)[0:1]
            pick = jnp.where(slot == rank, 1.0, 0.0) * named
            weight_ref[b * cap:(b + 1) * cap] = jnp.broadcast_to(
                jnp.sum(pick * share, axis=1, keepdims=True), (cap, 128))
            pick = pick.astype(jnp.bfloat16)
            pick_ref[b * cap:(b + 1) * cap] = pick
            rows_ref[b * cap:(b + 1) * cap] = jnp.dot(
                pick, x_ref[b], preferred_element_type=jnp.float32).astype(jnp.bfloat16)

    rows = rows_ref[...]
    gate = jnp.dot(rows, gate_ref[0, 0], preferred_element_type=jnp.float32)
    up = jnp.dot(rows, up_ref[0, 0], preferred_element_type=jnp.float32)
    hidden = (gate / (1.0 + jnp.exp(-gate)) * up).astype(jnp.bfloat16)
    product = jnp.dot(hidden, down_ref[0, 0], preferred_element_type=jnp.float32)

    @pl.when(j == 0)
    def _():
        acc_ref[...] = product

    @pl.when(j > 0)
    def _():
        acc_ref[...] += product

    @pl.when(j == last_j)
    def _():
        for b in range(line):
            own = slice(b * cap, (b + 1) * cap)
            weighted = (acc_ref[own] * weight_ref[own, 0:1]).astype(jnp.bfloat16)
            spread = lax.dot_general(pick_ref[own], weighted, (((0,), (0,)), ((), ())),
                                     preferred_element_type=jnp.float32)

            @pl.when(e == 0)
            def _():
                part_ref[b] = spread

            @pl.when(e == last_e)
            def _():
                o_ref[b] = (part_ref[b] + spread).astype(jnp.bfloat16)


def line_reduce(line, ways, parts, p_ref, t_ref, o_ref, from_left, from_right, sent, normed,
                right_sem, left_sem, right_recv, left_recv, out_sem, out_recv):
    ep, tp = lax.axis_index("ep"), lax.axis_index("tp")
    z = ep // PAIR
    tok, width = t_ref.shape
    rows, cols = tok // parts, width // ways
    barrier = pltpu.get_barrier_semaphore()

    @pl.when(z > 0)
    def _():
        pl.semaphore_signal(barrier, inc=1, device_id={"ep": ep - PAIR}, device_id_type=MESH)

    @pl.when(z < line - 1)
    def _():
        pl.semaphore_signal(barrier, inc=1, device_id={"ep": ep + PAIR}, device_id_type=MESH)

    for d in range(1, ways):
        pl.semaphore_signal(barrier, inc=1, device_id={"tp": lax.rem(tp + d, ways)}, device_id_type=MESH)
    pl.semaphore_wait(barrier, ways - 1 + jnp.where(z > 0, 1, 0) + jnp.where(z < line - 1, 1, 0))

    lanes = {1: (from_left, right_sem, right_recv), -1: (from_right, left_sem, left_recv)}

    def copy(way, source, block, part, target):
        landing, send, recv = lanes[way]
        piece = pl.ds(part * rows, rows)
        return pltpu.make_async_remote_copy(
            src_ref=source.at[block, piece], dst_ref=landing.at[block, piece],
            send_sem=send.at[block, part], recv_sem=recv.at[block, part],
            device_id={"ep": target}, device_id_type=MESH)

    def copy_out(d, part):
        peer = lax.rem(tp + d, ways)
        return pltpu.make_async_remote_copy(
            src_ref=normed.at[pl.ds(part * rows, rows), pl.ds(pl.multiple_of(peer * cols, cols), cols)],
            dst_ref=o_ref.at[pl.ds(pl.multiple_of(tp * tok + part * rows, rows), rows)],
            send_sem=out_sem.at[d - 1, part], recv_sem=out_recv.at[d - 1, part],
            device_id={"tp": peer}, device_id_type=MESH)

    for step in range(line - 1):
        for part in range(parts):
            piece = slice(part * rows, (part + 1) * rows)
            for way in (1, -1):
                block = line - 1 - step if way == 1 else step
                target = ep + way * PAIR
                ahead = z < block if way == 1 else z > block
                first = z == 0 if way == 1 else z == line - 1
                landing = lanes[way][0]

                @pl.when(first)
                def _():
                    copy(way, p_ref, block, part, target).start()

                @pl.when(ahead & jnp.logical_not(first))
                def _():
                    copy(way, sent, block, part, target).wait_recv()
                    sent[block, piece] = (p_ref[block, piece].astype(jnp.float32)
                                          + landing[block, piece].astype(jnp.float32)).astype(jnp.bfloat16)
                    copy(way, sent, block, part, target).start()

    for part in range(parts):
        piece = slice(part * rows, (part + 1) * rows)
        place = pl.ds(part * rows, rows)
        sent[z, place] = p_ref[z, place]

        @pl.when(z > 0)
        def _():
            copy(1, sent, z, part, ep).wait_recv()

        @pl.when(z < line - 1)
        def _():
            copy(-1, sent, z, part, ep).wait_recv()

        total = t_ref[piece].astype(jnp.float32) + p_ref[z, place].astype(jnp.float32)
        left = jnp.where(z > 0, from_left[z, place].astype(jnp.float32), 0.0)
        right = jnp.where(z < line - 1, from_right[z, place].astype(jnp.float32), 0.0)
        residual = (total + left + right).astype(jnp.bfloat16).astype(jnp.float32)
        inverse = lax.rsqrt(jnp.mean(residual * residual, axis=-1, keepdims=True) + EPS)
        normed[piece] = (residual * inverse).astype(jnp.bfloat16)
        for d in range(1, ways):
            copy_out(d, part).start()
        o_ref[pl.ds(pl.multiple_of(tp * tok + part * rows, rows), rows)] = normed[
            piece, pl.ds(pl.multiple_of(tp * cols, cols), cols)]

    for block in range(line):
        for way in (1, -1):
            ahead = z < block if way == 1 else z > block

            @pl.when(ahead)
            def _():
                for part in range(parts):
                    copy(way, sent, block, part, ep).wait_send()
    for part in range(parts):
        for d in range(1, ways):
            copy_out(d, part).wait_send()
            copy_out(d, part).wait_recv()


def route_shares(group_weight, expert_logit):
    share = jnp.exp(expert_logit)
    share = share / jnp.sum(share, axis=-1, keepdims=True)
    return group_weight[:, None] * share


def norm_in(tokens, norm_gain):
    tokens_f = tokens.astype(jnp.float32)
    inverse = lax.rsqrt(jnp.mean(tokens_f * tokens_f, axis=-1, keepdims=True) + EPS)
    return (tokens_f * inverse * norm_gain.astype(jnp.float32)).astype(jnp.bfloat16)


def on_line(tokens, norm_gain, expert_ids, group_weight, expert_logit, w_gate, w_up, w_down, final_gain):
    tok, width = tokens.shape
    top = expert_ids.shape[1]
    ep_size, ways = lax.axis_size("ep"), lax.axis_size("tp")
    line = ep_size // PAIR
    hidden = w_gate.shape[2]
    cap = 2 * tok * top // ep_size
    parts = 4
    count = ep_size * ways
    groups = [list(range(i, i + PAIR * ways)) for i in range(0, count, PAIR * ways)]
    gather = lambda w: lax.all_gather(w, ("ep", "tp"), axis_index_groups=groups)
    gates, ups, downs = gather(w_gate), gather(w_up), gather(w_down)

    x = norm_in(tokens, norm_gain)
    shares = route_shares(group_weight, expert_logit)
    meta = jnp.concatenate([expert_ids.astype(jnp.float32).T, shares.T, jnp.zeros((8 - 2 * top, tok), jnp.float32)])
    dma = pltpu.SemaphoreType.DMA
    every, every_meta = pl.pallas_call(
        functools.partial(line_gather, line, parts),
        out_shape=(jax.ShapeDtypeStruct((line, tok, width), jnp.bfloat16),
                   jax.ShapeDtypeStruct((line, 8, tok), jnp.float32)),
        in_specs=[VMEM] * 2, out_specs=(VMEM, VMEM),
        scratch_shapes=[dma((line, parts))] * 3 + [dma((line,))] * 3,
        cost_estimate=pl.CostEstimate(flops=60_000_000_000, bytes_accessed=8_000_000, transcendentals=0),
        compiler_params=pltpu.CompilerParams(collective_id=0, has_side_effects=True, vmem_limit_bytes=24 << 20),
        name="line_gather",
    )(x, meta)

    slots = line * cap
    weight_block = lambda shape: pl.BlockSpec((1, 1) + shape, lambda e, j: (e * ways + j, 0, 0, 0))
    whole = lambda shape: pl.BlockSpec(shape, lambda e, j: (0,) * len(shape))
    partial = pl.pallas_call(
        functools.partial(experts_kernel, line, cap),
        out_shape=jax.ShapeDtypeStruct((line, tok, width), jnp.bfloat16),
        grid=(PAIR, ways),
        in_specs=[whole((line, tok, width)), whole((line, 8, tok)), weight_block((width, hidden)),
                  weight_block((width, hidden)), weight_block((hidden, width))],
        out_specs=whole((line, tok, width)),
        scratch_shapes=[pltpu.VMEM((slots, width), jnp.bfloat16), pltpu.VMEM((slots, width), jnp.float32),
                        pltpu.VMEM((slots, tok), jnp.bfloat16), pltpu.VMEM((slots, 128), jnp.float32),
                        pltpu.VMEM((line, tok, width), jnp.float32)],
        cost_estimate=pl.CostEstimate(flops=14_000_000_000, bytes_accessed=30_000_000, transcendentals=1_000_000),
        compiler_params=pltpu.CompilerParams(vmem_limit_bytes=60 << 20),
        name="experts",
    )(every, every_meta, gates, ups, downs)

    block = pltpu.VMEM((line, tok, width), jnp.bfloat16)
    out = pl.pallas_call(
        functools.partial(line_reduce, line, ways, parts),
        out_shape=jax.ShapeDtypeStruct((ways * tok, width // ways), jnp.bfloat16),
        in_specs=[VMEM] * 2, out_specs=VMEM,
        scratch_shapes=[block, block, block, pltpu.VMEM((tok, width), jnp.bfloat16)]
        + [dma((line, parts))] * 4 + [dma((ways - 1, parts))] * 2,
        compiler_params=pltpu.CompilerParams(collective_id=1, has_side_effects=True, vmem_limit_bytes=40 << 20),
        name="line_reduce",
    )(partial, tokens)
    return (out.astype(jnp.float32) * final_gain.astype(jnp.float32)).astype(jnp.bfloat16)


def by_exchange(tokens, norm_gain, expert_ids, group_weight, expert_logit, w_gate, w_up, w_down, final_gain):
    tok_dev, width = tokens.shape
    per_token = expert_ids.shape[1]
    exp_dev = w_gate.shape[0]
    experts = exp_dev * lax.axis_size("ep")
    capacity = 2 * tok_dev * per_token // experts
    assigned = tok_dev * per_token
    tokens_f = tokens.astype(jnp.float32)
    normed_in = norm_in(tokens, norm_gain)
    flat_ids = expert_ids.reshape(assigned)
    onehot = (flat_ids[:, None] == jnp.arange(experts, dtype=jnp.int32)[None, :]).astype(jnp.int32)
    before = jnp.cumsum(onehot, axis=0) - onehot
    position = jnp.sum(before * onehot, axis=1) * experts + flat_ids
    owner_row = (
        jnp.zeros((capacity * experts,), jnp.int32)
        .at[position]
        .set(jnp.arange(assigned, dtype=jnp.int32) // per_token + 1)
    )
    source = normed_in[jnp.maximum(owner_row - 1, 0)]
    outgoing = jnp.where((owner_row > 0)[:, None], source, jnp.zeros_like(source)).reshape(capacity, experts, width)
    down_whole = lax.all_gather(w_down, "tp", axis=1, tiled=True)
    gate_whole = lax.all_gather(w_gate, "tp", axis=2, tiled=True)
    up_whole = lax.all_gather(w_up, "tp", axis=2, tiled=True)
    incoming = lax.all_to_all(outgoing, "ep", split_axis=1, concat_axis=1, tiled=True)
    senders = incoming.shape[1] // exp_dev
    arranged = incoming.reshape(capacity, senders, exp_dev, width)
    results = []
    for e in range(exp_dev):
        routed = arranged[:, :, e, :].reshape(capacity * senders, width)
        gate = jnp.dot(routed, gate_whole[e], preferred_element_type=jnp.float32)
        up = jnp.dot(routed, up_whole[e], preferred_element_type=jnp.float32)
        hidden = (jax.nn.silu(gate) * up).astype(jnp.bfloat16)
        product = jnp.dot(hidden, down_whole[e], preferred_element_type=jnp.float32).astype(jnp.bfloat16)
        results.append(product.reshape(capacity, senders, width))
    answer = jnp.stack(results, axis=2).reshape(capacity, senders * exp_dev, width)
    arrived = lax.all_to_all(answer, "ep", split_axis=1, concat_axis=1, tiled=True)
    picked = arrived.reshape(capacity * experts, width)[position].reshape(tok_dev, per_token, width)
    shares = route_shares(group_weight, expert_logit)
    mixture = tokens_f + jnp.sum(shares[:, :, None] * picked.astype(jnp.float32), axis=1)
    residual = mixture.astype(jnp.bfloat16)
    sliced = lax.all_to_all(residual, "tp", split_axis=1, concat_axis=0, tiled=True).astype(jnp.float32)
    squares = lax.psum(jnp.sum(sliced * sliced, axis=-1), "tp")
    inverse_out = lax.rsqrt(squares / width + EPS)
    return (sliced * inverse_out[:, None] * final_gain.astype(jnp.float32)).astype(jnp.bfloat16)


def solution(mesh):
    placed = (
        P(("ep", "tp"), None),
        P(),
        P(("ep", "tp"), None),
        P(("ep", "tp")),
        P(("ep", "tp"), None),
        P("ep", None, "tp"),
        P("ep", None, "tp"),
        P("ep", "tp", None),
        P("tp"),
    )

    def local(*args):
        ep_size = mesh.shape["ep"]
        short = ep_size % PAIR == 0 and 2 <= ep_size // PAIR <= 4 and args[5].shape[0] == 1
        return (on_line if short else by_exchange)(*args)

    return jax.shard_map(local, mesh=mesh, in_specs=placed, out_specs=P("ep", "tp"), check_vma=False)
```
